32 devices in a mesh: ep: 8 (over z, x), tp: 4 (over y, core).
Axes of the slice: x: 2, y: 2, z: 4, core: 2. Of those that a mesh axis runs over, the one named last changes fastest.
Arguments:
- first_batch: bfloat16 [4096, 2048], P(('ep', 'tp')), may hold values from -6 to 6
- mixer_gain: float32 [2048], replicated, may hold values from 0.1 to 1.9
- mixer_in: bfloat16 [2048, 512], P(None, 'tp'), may hold values from -0.125 to 0.125
- group_maps: bfloat16 [8, 64, 64], replicated, may hold values from -0.75 to 0.75
- pool_scale: float32 [512], replicated, may hold values from 0.1 to 1.9
- mixer_out: bfloat16 [512, 2048], P('tp'), may hold values from -0.25 to 0.25
- second_batch: bfloat16 [1024, 2048], P('ep'), may hold values from -6 to 6
- expert_gain: float32 [2048], replicated, may hold values from 0.1 to 1.9
- expert_choice: int32 [1024, 2], P('ep'), may hold values from 0 to 7, all different within a row; in each aligned block of 128 rows (0 to 127, 128 to 255, ...) at most 64 rows name the same one
- route_scores: float32 [1024, 2], P('ep'), may hold values from -6 to 6
- expert_gate: bfloat16 [8, 2048, 3584], P('ep', None, 'tp'), may hold values from -0.125 to 0.125
- expert_up: bfloat16 [8, 2048, 3584], P('ep', None, 'tp'), may hold values from -0.125 to 0.125
- expert_down: bfloat16 [8, 3584, 2048], P('ep', 'tp'), may hold values from -0.09375 to 0.09375
Outputs:
- mixed_first: bfloat16 [4096, 2048], P(('ep', 'tp'))
- experts_second: bfloat16 [1024, 2048], P('ep')
The draws below stay inside these ranges and needn't reach their ends.
Inputs may be any that keep to these rules, and one draw needn't show every extreme that they name: `expert_choice`: the two entries of a row differ. Within the rows of one device (aligned blocks of 128 rows) no expert is named more than 64 times, a bound that some block reaches there.
All inputs are finite; a program needn't handle non-finite values.
Results may differ from the reference program's by a relative error of at most 0.018.
Values may be sent and summed in bfloat16 or wider, within the bound.
A program may use at most 64 MiB of HBM per device.

```python
import math
import jax
import jax.numpy as jnp
import numpy as np
from jax import lax

D = 2048
POOL = 512
GROUP = 64
FF_E = 3584
TOP = 2
SEQS = 1
ROWS_B = 128
EXPERTS = 8
CAP = 64
GROUPS = 8
TOKENS_A = 4096
TOKENS_B = 1024
N_TP = 4


def block_scale(rng, extent, shards, smallest, largest):
    def one(dim, parts):
        steps = jax.random.uniform(jax.random.fold_in(jax.random.fold_in(rng, 6), dim), (parts,), jnp.float32, smallest / len(shards), largest / len(shards))
        return jnp.repeat(jnp.exp(steps), extent[dim] // parts).reshape((-1,) + (1,) * (len(extent) - dim - 1))

    level = one(*shards[0])
    for cut in shards[1:]:
        level = level * one(*cut)
    return level


def shared_out(key, own, number, rows, number_of, top, bound, skew):
    sequence = jax.random.permutation(key, number_of)
    packed, common = load_shares(number_of, rows * top, bound, skew, True), load_shares(number_of, rows * top, bound, skew, False)
    places = jnp.arange(number_of)

    def named(lengths, offset_by):
        used = int((lengths > 0).sum())
        fixed = max(1, used // 4)
        moved = fixed + (places - fixed + offset_by * (used - fixed)) % max(1, number_of - fixed)
        return jnp.zeros((number_of,), jnp.int32).at[sequence[jnp.where(places < fixed, places, moved)]].set(jnp.asarray(lengths, jnp.int32))

    lengths = jnp.where(number % 4 == 0, named(packed, number // 4), named(common, number - number // 4 - 1))
    mixed = jax.random.permutation(jax.random.fold_in(own, 3), number_of)
    source_of, receiver = mixed[0:number_of // 2 * 2:2], mixed[1:number_of // 2 * 2:2]
    room = jnp.minimum(lengths[source_of] - 1, bound - lengths[receiver]) // 2
    room = jnp.where((source_of == sequence[0]) | (receiver == sequence[0]) | (lengths[receiver] == 0), 0, jnp.maximum(room, 0))
    moved = jax.random.randint(jax.random.fold_in(own, 4), (number_of // 2,), 0, 1 << 20) % (room + 1)
    lengths = lengths.at[source_of].add(-moved).at[receiver].add(moved)
    members = jnp.searchsorted(jnp.cumsum(lengths), jnp.arange(rows * top), side="right").astype(jnp.int32)
    grid = members.reshape(top, rows).T
    grid = grid[jax.random.permutation(jax.random.fold_in(own, 1), rows)]
    offset_by = jax.random.randint(jax.random.fold_in(own, 2), (rows, 1), 0, top)
    return jnp.take_along_axis(grid, (jnp.arange(top)[None, :] + offset_by) % top, axis=1)


def load_shares(count, total, most, lean, full):
    portions = [(1 << 20) // math.isqrt(standing ** lean) + 1 for standing in range(1, count + 1)]
    largest = most if full else min(most, max(-(-total // count), total * portions[0] // sum(portions)))
    least = 1 if total - largest >= count - 1 else 0
    counts, rest = [largest] + [least] * (count - 1), total - largest - least * (count - 1)
    while rest > 0:
        free = [i for i in range(1, count) if counts[i] < largest] or [i for i in range(1, count) if counts[i] < most]
        whole, left = sum([portions[i] for i in free]), rest
        for i in free:
            extra = min(most - counts[i], max(1, left * portions[i] // whole), rest)
            counts[i] = counts[i] + extra
            rest = rest - extra
    return np.array(counts)


def noise(rng, dims, width, limit, split=(), held_as=jnp.bfloat16):
    loudness = block_scale(rng, dims, split, -0.22, 0.18) if split else 1.0
    array = jax.random.normal(rng, dims, jnp.float32) * width * loudness
    return jnp.minimum(jnp.maximum(array, -limit), limit).astype(held_as)


def setup_inputs(seed: int = 0) -> dict:
    keys = jax.random.split(jax.random.key(seed), 14)
    first_batch = noise(keys[0], (TOKENS_A, D), 1.0, 6.0, ((0, 32),))
    mixer_gain = jnp.clip(1.0 + 0.18 * jax.random.normal(keys[1], (D,), jnp.float32), 0.1, 1.9)
    mixer_in = noise(keys[2], (D, POOL), D ** -0.5, 0.125, ((1, 4),))
    group_maps = noise(keys[3], (GROUPS, GROUP, GROUP), GROUP ** -0.5, 0.75)
    pool_scale = jnp.clip(1.0 + 0.18 * jax.random.normal(keys[4], (POOL,), jnp.float32), 0.1, 1.9)
    mixer_out = noise(keys[5], (POOL, D), POOL ** -0.5, 0.25, ((0, 4),))
    second_batch = noise(keys[6], (TOKENS_B, D), 1.0, 6.0, ((0, 8),))
    expert_gain = jnp.clip(1.0 + 0.18 * jax.random.normal(keys[7], (D,), jnp.float32), 0.1, 1.9)
    expert_choice_keys = jax.random.split(jax.random.fold_in(keys[8], 1), TOKENS_B // ROWS_B)
    expert_choice_turns = jax.random.permutation(jax.random.fold_in(keys[8], 3), TOKENS_B // ROWS_B)
    expert_choice = jax.vmap(lambda own, number: shared_out(jax.random.fold_in(keys[8], 2), own, number, ROWS_B, EXPERTS, TOP, CAP, 1))(expert_choice_keys, expert_choice_turns).reshape((TOKENS_B, TOP))
    route_scores = noise(keys[9], (TOKENS_B, TOP), 1.5, 6.0, ((0, 8),), jnp.float32)
    expert_gate = noise(keys[10], (EXPERTS, D, FF_E), D ** -0.5, 0.125, ((0, 8), (2, 4)))
    expert_up = noise(keys[11], (EXPERTS, D, FF_E), D ** -0.5, 0.125, ((0, 8), (2, 4)))
    expert_down = noise(keys[12], (EXPERTS, FF_E, D), FF_E ** -0.5, 0.09375, ((0, 8), (1, 4)))
    return dict(first_batch=first_batch, mixer_gain=mixer_gain, mixer_in=mixer_in, group_maps=group_maps, pool_scale=pool_scale, mixer_out=mixer_out, second_batch=second_batch, expert_gain=expert_gain, expert_choice=expert_choice, route_scores=route_scores, expert_gate=expert_gate, expert_up=expert_up, expert_down=expert_down)


windows = (2, 4, 8, 16)
epsilon = 1e-06

def rms_scale(values, gain):
    floats = values.astype(jnp.float32)
    factor = lax.rsqrt(lax.optimization_barrier(jnp.mean(floats * floats, axis=-1, keepdims=True)) + epsilon)
    return (floats * factor * gain).astype(jnp.bfloat16)

def pool_centred(pooled_in):
    total = pooled_in.shape[0]
    seq_length = total // SEQS
    pooled_f32 = pooled_in.astype(jnp.float32).reshape(SEQS, seq_length, POOL)
    running = jnp.pad(jnp.cumsum(pooled_f32, axis=1), ((0, 0), (1, 0), (0, 0)))
    places = jnp.arange(seq_length, dtype=jnp.int32)
    pieces = []
    for group in range(POOL // GROUP):
        half_span = windows[group % 4] // 2
        upper_end = jnp.clip(places + half_span, 0, seq_length)
        lower_end = jnp.clip(places - half_span, 0, seq_length)
        group_sums = running[:, :, group * GROUP:(group + 1) * GROUP]
        window_sum = jnp.take(group_sums, upper_end, axis=1) - jnp.take(group_sums, lower_end, axis=1)
        window_count = (upper_end - lower_end).astype(jnp.float32)[None, :, None]
        pieces.append(window_sum / window_count - pooled_f32[:, :, group * GROUP:(group + 1) * GROUP])
    return jnp.concatenate(pieces, axis=-1).reshape(total, POOL).astype(jnp.bfloat16)

def reference(first_batch, mixer_gain, mixer_in, group_maps, pool_scale, mixer_out, second_batch, expert_gain, expert_choice, route_scores, expert_gate, expert_up, expert_down):
    normed_first = rms_scale(first_batch, mixer_gain)
    pooled_in = jnp.dot(normed_first, mixer_in, preferred_element_type=jnp.float32).astype(jnp.bfloat16)
    centred = pool_centred(pooled_in)
    group_count = POOL // GROUP
    grouped = jnp.einsum('tgc,gcd->tgd', centred.reshape(-1, group_count, GROUP).astype(jnp.float32), group_maps.astype(jnp.float32))
    grouped = (grouped.reshape(-1, POOL) * pool_scale).astype(jnp.bfloat16)
    mixed_first = jnp.dot(grouped, mixer_out, preferred_element_type=jnp.float32).astype(jnp.bfloat16)
    expert_count = expert_gate.shape[0]
    block_count = second_batch.shape[0] // ROWS_B
    normed_second = rms_scale(second_batch, expert_gain)
    chosen = expert_choice.reshape(block_count, ROWS_B * TOP)
    one_hot = (chosen[:, :, None] == jnp.arange(expert_count, dtype=jnp.int32)[None, None, :]).astype(jnp.int32)
    ranking = lax.optimization_barrier(jnp.sum(jnp.cumsum(one_hot, axis=1) * one_hot, axis=2)) - 1
    local_rows = jnp.arange(ROWS_B * TOP, dtype=jnp.int32) // TOP
    global_rows = local_rows[None, :] + (jnp.arange(block_count, dtype=jnp.int32) * ROWS_B)[:, None]
    block_index = jnp.arange(block_count, dtype=jnp.int32)[:, None]
    slot_place = ((chosen * block_count + block_index) * CAP + ranking).reshape(-1)
    slot_table = jnp.zeros((expert_count * block_count * CAP,), jnp.int32).at[slot_place].set(global_rows.reshape(-1) + 1)
    slot_table = slot_table.reshape(expert_count, block_count * CAP)
    split_size = FF_E // N_TP

    def one_expert(operands):
        row_index, gate_weight, up_weight, down_weight = operands
        live_rows = row_index > 0
        taken = jnp.where(live_rows[:, None], normed_second[jnp.maximum(row_index - 1, 0)], jnp.zeros((), jnp.bfloat16))
        gate_part = jnp.dot(taken, gate_weight, preferred_element_type=jnp.float32)
        up_part = jnp.dot(taken, up_weight, preferred_element_type=jnp.float32)
        hidden = (jax.nn.silu(gate_part) * up_part).astype(jnp.bfloat16)
        partial_value = jnp.einsum('rtf,tfd->trd', hidden.reshape(-1, N_TP, split_size).astype(jnp.float32), down_weight.reshape(N_TP, split_size, D).astype(jnp.float32))
        rounded = lax.optimization_barrier(partial_value.astype(jnp.bfloat16))
        return lax.optimization_barrier(jnp.sum(rounded.astype(jnp.float32), axis=0)).astype(jnp.bfloat16)
    results = lax.map(one_expert, (slot_table, expert_gate, expert_up, expert_down))
    flat_results = results.reshape(expert_count * block_count * CAP, D)
    picked = flat_results[slot_place].reshape(-1, TOP, D).astype(jnp.float32)
    weight_first = jax.nn.sigmoid(route_scores[:, 0] - route_scores[:, 1])[:, None]
    experts_second = (weight_first * picked[:, 0] + (1.0 - weight_first) * picked[:, 1]).astype(jnp.bfloat16)
    return (mixed_first, experts_second)
```

```python
import jax
import jax.numpy as jnp
from jax import lax
from jax.experimental import pallas as pl
from jax.experimental.pallas import tpu as pltpu
from jax.sharding import PartitionSpec as P

GROUP = 64
SEQS = 1


epsilon = 1e-06


def extended(block, sides, width):
    for axis, dim in sides:
        count = lax.axis_size(axis)
        forward = [(i, i + 1) for i in range(count - 1)]
        backward = [(target, source) for source, target in forward]
        low = lax.ppermute(
            lax.slice_in_dim(block, block.shape[dim] - width, None, axis=dim), axis, forward
        )
        high = lax.ppermute(lax.slice_in_dim(block, 0, width, axis=dim), axis, backward)
        block = jnp.concatenate([low, block, high], axis=dim)
    return block


def rms_scale(values, gain):
    floats = values.astype(jnp.float32)
    factor = lax.rsqrt(jnp.mean(floats * floats, axis=-1, keepdims=True) + epsilon)
    return (floats * factor * gain).astype(jnp.bfloat16)


def mixer_half(first_batch, mixer_gain, mixer_in, group_maps, pool_scale, mixer_out):
    count_rows = first_batch.shape[0]
    normed = rms_scale(first_batch, mixer_gain)
    pooled_in = jnp.dot(
        normed,
        lax.all_gather(mixer_in, "tp", axis=1, tiled=True),
        preferred_element_type=jnp.float32,
    ).astype(jnp.bfloat16)
    channels = pooled_in.shape[1]
    padded = extended(pooled_in, ((("ep", "tp"), 0),), 8).astype(jnp.float32)
    devices = lax.axis_size("ep") * lax.axis_size("tp")
    seq_length = count_rows * devices // SEQS
    first_row = (lax.axis_index("ep") * lax.axis_size("tp") + lax.axis_index("tp")) * count_rows
    places = first_row + jnp.arange(count_rows, dtype=jnp.int32)
    own_seq = places // seq_length
    group_of = jnp.arange(channels, dtype=jnp.int32) // GROUP
    half_span = jnp.left_shift(jnp.ones_like(group_of), group_of % 4)
    window_sum = jnp.zeros((count_rows, channels), jnp.float32)
    window_count = jnp.zeros((count_rows, channels), jnp.float32)
    for offset in range(-8, 8):
        inside = (
            ((places + offset) // seq_length == own_seq)[:, None]
            & (offset >= -half_span)[None, :]
            & (offset < half_span)[None, :]
        )
        window_sum = window_sum + jnp.where(
            inside, padded[8 + offset : 8 + offset + count_rows], 0.0
        )
        window_count = window_count + inside.astype(jnp.float32)
    centred = (window_sum / window_count - padded[8 : 8 + count_rows]).astype(jnp.bfloat16)
    group_count = group_maps.shape[0]
    identity = jnp.eye(group_count, dtype=jnp.bfloat16)
    block_map = jnp.einsum("gcd,gh->gchd", group_maps, identity).reshape(channels, channels)
    grouped = (jnp.dot(centred, block_map, preferred_element_type=jnp.float32) * pool_scale).astype(
        jnp.bfloat16
    )
    mixed_out = jnp.dot(
        grouped,
        lax.all_gather(mixer_out, "tp", axis=0, tiled=True),
        preferred_element_type=jnp.float32,
    )
    return mixed_out.astype(jnp.bfloat16)


def expert_half(
    second_batch, expert_gain, expert_choice, route_scores, expert_gate, expert_up, expert_down
):
    row_count = second_batch.shape[0]
    model_width = second_batch.shape[1]
    experts = lax.axis_size("ep")
    tp_count = lax.axis_size("tp")
    capacity = 4 * row_count // experts
    share = capacity // tp_count
    normed = rms_scale(second_batch, expert_gain)
    chosen = expert_choice.reshape(-1)
    one_hot = (chosen[:, None] == jnp.arange(experts, dtype=jnp.int32)[None, :]).astype(jnp.int32)
    ranking = jnp.sum(jnp.cumsum(one_hot, axis=0) * one_hot, axis=1) - 1
    slot_place = ranking * experts + chosen
    source_row = jnp.arange(chosen.shape[0], dtype=jnp.int32) // expert_choice.shape[1]
    slot_table = jnp.zeros((capacity * experts,), jnp.int32).at[slot_place].set(source_row + 1)
    outgoing = jnp.where(
        (slot_table > 0)[:, None],
        normed[jnp.maximum(slot_table - 1, 0)],
        jnp.zeros((), jnp.bfloat16),
    )
    outgoing = outgoing.reshape(capacity, experts, model_width)
    portion = lax.dynamic_slice_in_dim(outgoing, lax.axis_index("tp") * share, share, 0)
    arrived_part = lax.all_to_all(portion, "ep", split_axis=1, concat_axis=1, tiled=True)
    arrived = lax.all_gather(arrived_part, "tp", axis=0, tiled=True)
    incoming = arrived.reshape(capacity * experts, model_width)
    gate_weight = expert_gate[0]
    up_weight = expert_up[0]
    down_weight = expert_down[0]
    gate_part = jnp.dot(incoming, gate_weight, preferred_element_type=jnp.float32)
    up_part = jnp.dot(incoming, up_weight, preferred_element_type=jnp.float32)
    hidden = (jax.nn.silu(gate_part) * up_part).astype(jnp.bfloat16)
    summed = lax.psum_scatter(
        jnp.dot(hidden, down_weight, preferred_element_type=jnp.float32).astype(jnp.bfloat16),
        "tp",
        scatter_dimension=0,
        tiled=True,
    )
    finished = summed.reshape(share, experts, model_width)
    returned = lax.all_to_all(finished, "ep", split_axis=1, concat_axis=1, tiled=True)
    every_slot = lax.all_gather(returned, "tp", axis=0, tiled=True).reshape(
        capacity * experts, model_width
    )
    picked = every_slot[slot_place].reshape(row_count, -1, model_width)
    weight_first = jax.nn.sigmoid(route_scores[:, 0] - route_scores[:, 1])[:, None]
    blended = weight_first * picked[:, 0].astype(jnp.float32) + (1.0 - weight_first) * picked[
        :, 1
    ].astype(jnp.float32)
    return blended.astype(jnp.bfloat16)


MESH = pl.DeviceIdType.MESH
VMEM_LIMIT = 40 * 1024 * 1024


def greet(peers):
    barrier = pltpu.get_barrier_semaphore()
    for peer in peers:
        pl.semaphore_signal(barrier, inc=1, device_id=peer, device_id_type=MESH)
    pl.semaphore_wait(barrier, len(peers))


def places_of(count):
    row = lax.axis_index("ep")
    col = lax.axis_index("tp")
    partner = col + 1 - 2 * (col % 2)
    across = (col + 2) % 4
    others = [((row + k) % count, col) for k in range(1, count)]
    return row, col, partner, across, others


def remote(source, target, send, recv, device):
    return pltpu.make_async_remote_copy(
        src_ref=source,
        dst_ref=target,
        send_sem=send,
        recv_sem=recv,
        device_id=device,
        device_id_type=MESH,
    )


def dispatch_kernel(count, portion, result, landed, send, recv, local):
    row, col, partner, across, others = places_of(count)
    greet(others + [(row, partner), (row, across)])
    firsts = [None]
    for k in range(1, count):
        copy = remote(
            portion.at[(row + k) % count], landed.at[row, col], send.at[0, k], recv.at[0, k],
            ((row + k) % count, col),
        )
        copy.start()
        firsts.append(copy)
    own = pltpu.make_async_copy(portion.at[row], landed.at[row, col], local.at[0])
    own.start()
    own.wait()
    sides, ys, corners = [], [], []
    lag = 2
    for k in range(count + lag):
        if k < count:
            source = (row + count - k) % count
            if k > 0:
                firsts[k].wait_recv()
            block = landed.at[source, col]
            y = remote(block, block, send.at[1, k], recv.at[1, k], (row, across))
            y.start()
            side = remote(block, block, send.at[2, k], recv.at[2, k], (row, partner))
            side.start()
            ys.append(y)
            sides.append(side)
        if k >= lag:
            j = k - lag
            source = (row + count - j) % count
            ys[j].wait_recv()
            block = landed.at[source, across]
            corner = remote(block, block, send.at[3, j], recv.at[3, j], (row, partner))
            corner.start()
            corners.append(corner)
    for k in range(count):
        sides[k].wait_recv()
        corners[k].wait_recv()
    out = pltpu.make_async_copy(landed, result, local.at[1])
    out.start()
    for k in range(count):
        if k > 0:
            firsts[k].wait_send()
        ys[k].wait_send()
        sides[k].wait_send()
        corners[k].wait_send()
    out.wait()


def dispatch(portion):
    count, share, width = portion.shape
    return pl.pallas_call(
        lambda *refs: dispatch_kernel(count, *refs),
        out_shape=jax.ShapeDtypeStruct((count, 4, share, width), portion.dtype),
        in_specs=[pl.BlockSpec(memory_space=pltpu.VMEM)],
        out_specs=pl.BlockSpec(memory_space=pl.ANY),
        scratch_shapes=[
            pltpu.VMEM((count, 4, share, width), portion.dtype),
            pltpu.SemaphoreType.DMA((4, count)),
            pltpu.SemaphoreType.DMA((4, count)),
            pltpu.SemaphoreType.DMA((2,)),
        ],
        compiler_params=pltpu.CompilerParams(
            collective_id=0, has_side_effects=True, vmem_limit_bytes=VMEM_LIMIT
        ),
        cost_estimate=pl.CostEstimate(flops=10**9, bytes_accessed=2**21, transcendentals=0),
        name="dispatch",
    )(portion)


def combine_kernel(
    count, part, weights, out, side_y, side_own, sums_y, from_y, sums, slots, pieces,
    send, recv, send_out, recv_out,
):
    row, col, partner, across, others = places_of(count)
    greet(others + [(row, partner), (row, across)])
    quarter = part.shape[2] // 4
    corner = (partner + 2) % 4

    def columns(q):
        return pl.ds(pl.multiple_of(q * quarter, quarter), quarter)

    order = list(range(1, count)) + [0]
    to_side, to_own, to_y, to_ep = {}, {}, {}, {}
    for k in order:
        target = (row + k) % count
        to_side[k] = remote(
            part.at[target, :, columns(corner)], side_y.at[k], send.at[0, k], recv.at[0, k],
            (row, partner),
        )
        to_side[k].start()
        to_own[k] = remote(
            part.at[target, :, columns(partner)], side_own.at[k], send.at[1, k], recv.at[1, k],
            (row, partner),
        )
        to_own[k].start()

    def start_y(k):
        to_y[k] = remote(
            sums_y.at[k], from_y.at[k], send.at[2, k], recv.at[2, k], (row, across)
        )
        to_y[k].start()

    def start_ep(k):
        if k:
            to_ep[k] = remote(
                sums.at[k], slots.at[row], send.at[3, k], recv.at[3, k],
                ((row + k) % count, col),
            )
            to_ep[k].start()

    for i, k in enumerate(order):
        target = (row + k) % count
        to_side[k].wait_recv()
        sums_y[k] = (
            part[target, :, columns(across)].astype(jnp.float32)
            + side_y[k].astype(jnp.float32)
        ).astype(jnp.bfloat16)
        if i:
            start_y(order[i - 1])
    to_own[order[0]].wait_recv()
    start_y(order[-1])
    for i, k in enumerate(order):
        target = (row + k) % count
        if i:
            to_own[k].wait_recv()
        mine = part[target, :, columns(col)].astype(jnp.float32) + side_own[k].astype(
            jnp.float32
        )
        to_y[k].wait_recv()
        total = (mine + from_y[k].astype(jnp.float32)).astype(jnp.bfloat16)
        if k:
            sums[k] = total
            start_ep(k)
        else:
            slots[row] = total
    table = weights[...]
    high = table.astype(jnp.bfloat16)
    low = (table - high.astype(jnp.float32)).astype(jnp.bfloat16)
    for k in order[:-1]:
        to_ep[k].wait_recv()
    rows = slots[...].reshape(-1, quarter)
    blended = jnp.dot(high, rows, preferred_element_type=jnp.float32) + jnp.dot(
        low, rows, preferred_element_type=jnp.float32
    )
    pieces[col] = blended.astype(jnp.bfloat16)
    own = pieces.at[col]
    out_y = remote(own, own, send_out.at[0], recv_out.at[0], (row, across))
    out_y.start()
    out_side = remote(own, own, send_out.at[1], recv_out.at[1], (row, partner))
    out_side.start()
    out[:, columns(col)] = pieces[col]
    out_y.wait_recv()
    other = pieces.at[across]
    out_corner = remote(other, other, send_out.at[2], recv_out.at[2], (row, partner))
    out_corner.start()
    out[:, columns(across)] = pieces[across]
    out_side.wait_recv()
    out[:, columns(partner)] = pieces[partner]
    for k in order:
        to_side[k].wait_send()
        to_own[k].wait_send()
        to_y[k].wait_send()
        if k:
            to_ep[k].wait_send()
    out_corner.wait_recv()
    out[:, columns(corner)] = pieces[corner]
    out_y.wait_send()
    out_side.wait_send()
    out_corner.wait_send()


def combine(part, weights):
    count, capacity, width = part.shape
    rows = weights.shape[0]
    quarter = width // 4
    chunk = pltpu.VMEM((count, capacity, quarter), jnp.bfloat16)
    return pl.pallas_call(
        lambda *refs: combine_kernel(count, *refs),
        out_shape=jax.ShapeDtypeStruct((rows, width), jnp.bfloat16),
        in_specs=[pl.BlockSpec(memory_space=pltpu.VMEM)] * 2,
        out_specs=pl.BlockSpec(memory_space=pltpu.VMEM),
        scratch_shapes=[chunk] * 6
        + [
            pltpu.VMEM((4, rows, quarter), jnp.bfloat16),
            pltpu.SemaphoreType.DMA((4, count)),
            pltpu.SemaphoreType.DMA((4, count)),
            pltpu.SemaphoreType.DMA((3,)),
            pltpu.SemaphoreType.DMA((3,)),
        ],
        compiler_params=pltpu.CompilerParams(
            collective_id=1, has_side_effects=True, vmem_limit_bytes=VMEM_LIMIT
        ),
        cost_estimate=pl.CostEstimate(flops=10**9, bytes_accessed=2**21, transcendentals=0),
        name="combine",
    )(part, weights)


def expert_half_kernels(
    second_batch, expert_gain, expert_choice, route_scores, expert_gate, expert_up, expert_down
):
    row_count, model_width = second_batch.shape
    experts = lax.axis_size("ep")
    capacity = 4 * row_count // experts
    share = capacity // 4
    normed = rms_scale(second_batch, expert_gain)
    names = jnp.arange(experts, dtype=jnp.int32)
    is_first = expert_choice[:, 0:1] == names[None, :]
    is_second = expert_choice[:, 1:2] == names[None, :]
    named = is_first | is_second
    rows = jnp.arange(row_count, dtype=jnp.int32)
    before = (rows[None, :] < rows[:, None]).astype(jnp.bfloat16)
    rank = jnp.dot(
        before, named.astype(jnp.bfloat16), preferred_element_type=jnp.float32
    ).astype(jnp.int32)
    rank = jnp.where(named, rank, -1)
    places = lax.axis_index("tp") * share + jnp.arange(share, dtype=jnp.int32)
    pick = (rank.T[:, None, :] == places[None, :, None]).astype(jnp.bfloat16)
    portion = (
        jnp.dot(
            pick.reshape(experts * share, row_count), normed, preferred_element_type=jnp.float32
        )
        .astype(jnp.bfloat16)
        .reshape(experts, share, model_width)
    )
    incoming = dispatch(portion).reshape(experts * capacity, model_width)
    gate_part = jnp.dot(incoming, expert_gate[0], preferred_element_type=jnp.float32)
    up_part = jnp.dot(incoming, expert_up[0], preferred_element_type=jnp.float32)
    hidden = (jax.nn.silu(gate_part) * up_part).astype(jnp.bfloat16)
    part = jnp.dot(hidden, expert_down[0], preferred_element_type=jnp.float32).astype(
        jnp.bfloat16
    )
    weight_first = jax.nn.sigmoid(route_scores[:, 0] - route_scores[:, 1])[:, None]
    weight = jnp.where(is_first, weight_first, 1.0 - weight_first)
    slot = jnp.arange(capacity, dtype=jnp.int32)
    table = jnp.where(rank[:, :, None] == slot[None, None, :], weight[:, :, None], 0.0)
    return combine(
        part.reshape(experts, capacity, model_width),
        table.reshape(row_count, experts * capacity),
    )


def per_device(
    first_batch,
    mixer_gain,
    mixer_in,
    group_maps,
    pool_scale,
    mixer_out,
    second_batch,
    expert_gain,
    expert_choice,
    route_scores,
    expert_gate,
    expert_up,
    expert_down,
):
    mixed_first = mixer_half(first_batch, mixer_gain, mixer_in, group_maps, pool_scale, mixer_out)
    small = lax.axis_size("tp") == 4 and lax.axis_size("ep") <= 8
    experts_second = (expert_half_kernels if small else expert_half)(
        second_batch, expert_gain, expert_choice, route_scores, expert_gate, expert_up, expert_down
    )
    return (mixed_first, experts_second)


def solution(mesh):
    placed = (
        P(("ep", "tp"), None),
        P(),
        P(None, "tp"),
        P(),
        P(),
        P("tp", None),
        P("ep", None),
        P(),
        P("ep", None),
        P("ep", None),
        P("ep", None, "tp"),
        P("ep", None, "tp"),
        P("ep", "tp", None),
    )
    return jax.shard_map(
        per_device,
        mesh=mesh,
        in_specs=placed,
        out_specs=(P(("ep", "tp"), None), P("ep", None)),
        check_vma=False,
    )
```

```python
import jax
import jax.numpy as jnp
from jax import lax
from jax.experimental import pallas as pl
from jax.experimental.pallas import tpu as pltpu
from jax.sharding import PartitionSpec as P

GROUP = 64
SEQS = 1


epsilon = 1e-06


def extended(block, sides, width):
    for axis, dim in sides:
        count = lax.axis_size(axis)
        forward = [(i, i + 1) for i in range(count - 1)]
        backward = [(target, source) for source, target in forward]
        low = lax.ppermute(
            lax.slice_in_dim(block, block.shape[dim] - width, None, axis=dim), axis, forward
        )
        high = lax.ppermute(lax.slice_in_dim(block, 0, width, axis=dim), axis, backward)
        block = jnp.concatenate([low, block, high], axis=dim)
    return block


def rms_scale(values, gain):
    floats = values.astype(jnp.float32)
    factor = lax.rsqrt(jnp.mean(floats * floats, axis=-1, keepdims=True) + epsilon)
    return (floats * factor * gain).astype(jnp.bfloat16)


def mixer_half(first_batch, mixer_gain, mixer_in, group_maps, pool_scale, mixer_out):
    count_rows = first_batch.shape[0]
    normed = rms_scale(first_batch, mixer_gain)
    pooled_in = jnp.dot(
        normed,
        mixer_in,
        preferred_element_type=jnp.float32,
    ).astype(jnp.bfloat16)
    channels = pooled_in.shape[1]
    padded = extended(pooled_in, ((("ep", "tp"), 0),), 8).astype(jnp.float32)
    devices = lax.axis_size("ep") * lax.axis_size("tp")
    seq_length = count_rows * devices // SEQS
    first_row = (lax.axis_index("ep") * lax.axis_size("tp") + lax.axis_index("tp")) * count_rows
    places = first_row + jnp.arange(count_rows, dtype=jnp.int32)
    own_seq = places // seq_length
    group_of = jnp.arange(channels, dtype=jnp.int32) // GROUP
    half_span = jnp.left_shift(jnp.ones_like(group_of), group_of % 4)
    window_sum = jnp.zeros((count_rows, channels), jnp.float32)
    window_count = jnp.zeros((count_rows, channels), jnp.float32)
    for offset in range(-8, 8):
        inside = (
            ((places + offset) // seq_length == own_seq)[:, None]
            & (offset >= -half_span)[None, :]
            & (offset < half_span)[None, :]
        )
        window_sum = window_sum + jnp.where(
            inside, padded[8 + offset : 8 + offset + count_rows], 0.0
        )
        window_count = window_count + inside.astype(jnp.float32)
    centred = (window_sum / window_count - padded[8 : 8 + count_rows]).astype(jnp.bfloat16)
    group_count = group_maps.shape[0]
    identity = jnp.eye(group_count, dtype=jnp.bfloat16)
    block_map = jnp.einsum("gcd,gh->gchd", group_maps, identity).reshape(channels, channels)
    grouped = (jnp.dot(centred, block_map, preferred_element_type=jnp.float32) * pool_scale).astype(
        jnp.bfloat16
    )
    mixed_out = jnp.dot(
        grouped,
        mixer_out,
        preferred_element_type=jnp.float32,
    )
    return mixed_out.astype(jnp.bfloat16)


def expert_half(
    second_batch, expert_gain, expert_choice, route_scores, expert_gate, expert_up, expert_down
):
    row_count = second_batch.shape[0]
    model_width = second_batch.shape[1]
    experts = lax.axis_size("ep")
    tp_count = lax.axis_size("tp")
    capacity = 4 * row_count // experts
    share = capacity // tp_count
    normed = rms_scale(second_batch, expert_gain)
    chosen = expert_choice.reshape(-1)
    one_hot = (chosen[:, None] == jnp.arange(experts, dtype=jnp.int32)[None, :]).astype(jnp.int32)
    ranking = jnp.sum(jnp.cumsum(one_hot, axis=0) * one_hot, axis=1) - 1
    slot_place = ranking * experts + chosen
    source_row = jnp.arange(chosen.shape[0], dtype=jnp.int32) // expert_choice.shape[1]
    slot_table = jnp.zeros((capacity * experts,), jnp.int32).at[slot_place].set(source_row + 1)
    outgoing = jnp.where(
        (slot_table > 0)[:, None],
        normed[jnp.maximum(slot_table - 1, 0)],
        jnp.zeros((), jnp.bfloat16),
    )
    outgoing = outgoing.reshape(capacity, experts, model_width)
    portion = lax.dynamic_slice_in_dim(outgoing, lax.axis_index("tp") * share, share, 0)
    arrived_part = lax.all_to_all(portion, "ep", split_axis=1, concat_axis=1, tiled=True)
    arrived = lax.all_gather(arrived_part, "tp", axis=0, tiled=True)
    incoming = arrived.reshape(capacity * experts, model_width)
    gate_weight = expert_gate[0]
    up_weight = expert_up[0]
    down_weight = expert_down[0]
    gate_part = jnp.dot(incoming, gate_weight, preferred_element_type=jnp.float32)
    up_part = jnp.dot(incoming, up_weight, preferred_element_type=jnp.float32)
    hidden = (jax.nn.silu(gate_part) * up_part).astype(jnp.bfloat16)
    summed = lax.psum_scatter(
        jnp.dot(hidden, down_weight, preferred_element_type=jnp.float32).astype(jnp.bfloat16),
        "tp",
        scatter_dimension=0,
        tiled=True,
    )
    finished = summed.reshape(share, experts, model_width)
    returned = lax.all_to_all(finished, "ep", split_axis=1, concat_axis=1, tiled=True)
    every_slot = lax.all_gather(returned, "tp", axis=0, tiled=True).reshape(
        capacity * experts, model_width
    )
    picked = every_slot[slot_place].reshape(row_count, -1, model_width)
    weight_first = jax.nn.sigmoid(route_scores[:, 0] - route_scores[:, 1])[:, None]
    blended = weight_first * picked[:, 0].astype(jnp.float32) + (1.0 - weight_first) * picked[
        :, 1
    ].astype(jnp.float32)
    return blended.astype(jnp.bfloat16)


MESH = pl.DeviceIdType.MESH
VMEM_LIMIT = 40 * 1024 * 1024


def greet(peers):
    barrier = pltpu.get_barrier_semaphore()
    for peer in peers:
        pl.semaphore_signal(barrier, inc=1, device_id=peer, device_id_type=MESH)
    pl.semaphore_wait(barrier, len(peers))


def places_of(count):
    row = lax.axis_index("ep")
    col = lax.axis_index("tp")
    partner = col + 1 - 2 * (col % 2)
    across = (col + 2) % 4
    others = [((row + k) % count, col) for k in range(1, count)]
    return row, col, partner, across, others


def remote(source, target, send, recv, device):
    return pltpu.make_async_remote_copy(
        src_ref=source,
        dst_ref=target,
        send_sem=send,
        recv_sem=recv,
        device_id=device,
        device_id_type=MESH,
    )


def dispatch_kernel(
    count, portion, w_in, w_out, result, full_in, full_out, landed, held_in, held_out,
    send, recv, local, send_w, recv_w,
):
    row, col, partner, across, others = places_of(count)
    greet(others + [(row, partner), (row, across)])
    firsts = [None]
    for k in range(1, count):
        copy = remote(
            portion.at[(row + k) % count], landed.at[row, col], send.at[0, k], recv.at[0, k],
            ((row + k) % count, col),
        )
        copy.start()
        firsts.append(copy)

    def piece(which, index):
        if which == 0:
            size = w_in.shape[1]
            return held_in.at[:, pl.ds(pl.multiple_of(index * size, size), size)]
        size = w_out.shape[0]
        return held_out.at[pl.ds(pl.multiple_of(index * size, size), size), :]

    weights = []
    for which, source in ((0, w_in), (1, w_out)):
        here = pltpu.make_async_copy(source, piece(which, col), local.at[2 + which])
        here.start()
        y = remote(
            source, piece(which, col), send_w.at[which, 0], recv_w.at[which, 0], (row, across)
        )
        y.start()
        side = remote(
            source, piece(which, col), send_w.at[which, 1], recv_w.at[which, 1], (row, partner)
        )
        side.start()
        weights.append((here, y, side))
    own = pltpu.make_async_copy(portion.at[row], landed.at[row, col], local.at[0])
    own.start()
    own.wait()
    sides, ys, corners = [], [], []
    lag = 2
    for k in range(count + lag):
        if k < count:
            source = (row + count - k) % count
            if k > 0:
                firsts[k].wait_recv()
            block = landed.at[source, col]
            y = remote(block, block, send.at[1, k], recv.at[1, k], (row, across))
            y.start()
            side = remote(block, block, send.at[2, k], recv.at[2, k], (row, partner))
            side.start()
            ys.append(y)
            sides.append(side)
        if k >= lag:
            j = k - lag
            source = (row + count - j) % count
            ys[j].wait_recv()
            block = landed.at[source, across]
            corner = remote(block, block, send.at[3, j], recv.at[3, j], (row, partner))
            corner.start()
            corners.append(corner)
    for k in range(count):
        sides[k].wait_recv()
        corners[k].wait_recv()
    out = pltpu.make_async_copy(landed, result, local.at[1])
    out.start()
    corner_w = []
    for which in (0, 1):
        weights[which][1].wait_recv()
        block = piece(which, across)
        copy = remote(block, block, send_w.at[which, 2], recv_w.at[which, 2], (row, partner))
        copy.start()
        corner_w.append(copy)
    outs = []
    for which, held, full in ((0, held_in, full_in), (1, held_out, full_out)):
        here, y, side = weights[which]
        here.wait()
        side.wait_recv()
        corner_w[which].wait_recv()
        copy = pltpu.make_async_copy(held, full, local.at[4 + which])
        copy.start()
        outs.append(copy)
    for which in (0, 1):
        weights[which][1].wait_send()
        weights[which][2].wait_send()
        corner_w[which].wait_send()
        outs[which].wait()
    for k in range(count):
        if k > 0:
            firsts[k].wait_send()
        ys[k].wait_send()
        sides[k].wait_send()
        corners[k].wait_send()
    out.wait()


def dispatch(portion, w_in, w_out):
    count, share, width = portion.shape
    shape_in = (w_in.shape[0], 4 * w_in.shape[1])
    shape_out = (4 * w_out.shape[0], w_out.shape[1])
    return pl.pallas_call(
        lambda *refs: dispatch_kernel(count, *refs),
        out_shape=(
            jax.ShapeDtypeStruct((count, 4, share, width), portion.dtype),
            jax.ShapeDtypeStruct(shape_in, w_in.dtype),
            jax.ShapeDtypeStruct(shape_out, w_out.dtype),
        ),
        in_specs=[pl.BlockSpec(memory_space=pltpu.VMEM)] * 3,
        out_specs=[pl.BlockSpec(memory_space=pl.ANY)] * 3,
        scratch_shapes=[
            pltpu.VMEM((count, 4, share, width), portion.dtype),
            pltpu.VMEM(shape_in, w_in.dtype),
            pltpu.VMEM(shape_out, w_out.dtype),
            pltpu.SemaphoreType.DMA((4, count)),
            pltpu.SemaphoreType.DMA((4, count)),
            pltpu.SemaphoreType.DMA((6,)),
            pltpu.SemaphoreType.DMA((2, 3)),
            pltpu.SemaphoreType.DMA((2, 3)),
        ],
        compiler_params=pltpu.CompilerParams(
            collective_id=0, has_side_effects=True, vmem_limit_bytes=VMEM_LIMIT
        ),
        cost_estimate=pl.CostEstimate(flops=10**9, bytes_accessed=2**21, transcendentals=0),
        name="dispatch",
    )(portion, w_in, w_out)


def combine_kernel(
    count, part, weights, out, side_y, side_own, sums_y, from_y, sums, slots, pieces,
    send, recv, send_out, recv_out,
):
    row, col, partner, across, others = places_of(count)
    greet(others + [(row, partner), (row, across)])
    quarter = part.shape[2] // 4
    corner = (partner + 2) % 4

    def columns(q):
        return pl.ds(pl.multiple_of(q * quarter, quarter), quarter)

    order = list(range(1, count)) + [0]
    to_side, to_own, to_y, to_ep = {}, {}, {}, {}
    for k in order:
        target = (row + k) % count
        to_side[k] = remote(
            part.at[target, :, columns(corner)], side_y.at[k], send.at[0, k], recv.at[0, k],
            (row, partner),
        )
        to_side[k].start()
        to_own[k] = remote(
            part.at[target, :, columns(partner)], side_own.at[k], send.at[1, k], recv.at[1, k],
            (row, partner),
        )
        to_own[k].start()

    def start_y(k):
        to_y[k] = remote(
            sums_y.at[k], from_y.at[k], send.at[2, k], recv.at[2, k], (row, across)
        )
        to_y[k].start()

    def start_ep(k):
        if k:
            to_ep[k] = remote(
                sums.at[k], slots.at[row], send.at[3, k], recv.at[3, k],
                ((row + k) % count, col),
            )
            to_ep[k].start()

    for i, k in enumerate(order):
        target = (row + k) % count
        to_side[k].wait_recv()
        sums_y[k] = (
            part[target, :, columns(across)].astype(jnp.float32)
            + side_y[k].astype(jnp.float32)
        ).astype(jnp.bfloat16)
        if i:
            start_y(order[i - 1])
    to_own[order[0]].wait_recv()
    start_y(order[-1])
    for i, k in enumerate(order):
        target = (row + k) % count
        if i:
            to_own[k].wait_recv()
        mine = part[target, :, columns(col)].astype(jnp.float32) + side_own[k].astype(
            jnp.float32
        )
        to_y[k].wait_recv()
        total = (mine + from_y[k].astype(jnp.float32)).astype(jnp.bfloat16)
        if k:
            sums[k] = total
            start_ep(k)
        else:
            slots[row] = total
    table = weights[...]
    high = table.astype(jnp.bfloat16)
    low = (table - high.astype(jnp.float32)).astype(jnp.bfloat16)
    for k in order[:-1]:
        to_ep[k].wait_recv()
    rows = slots[...].reshape(-1, quarter)
    blended = jnp.dot(high, rows, preferred_element_type=jnp.float32) + jnp.dot(
        low, rows, preferred_element_type=jnp.float32
    )
    pieces[col] = blended.astype(jnp.bfloat16)
    own = pieces.at[col]
    out_y = remote(own, own, send_out.at[0], recv_out.at[0], (row, across))
    out_y.start()
    out_side = remote(own, own, send_out.at[1], recv_out.at[1], (row, partner))
    out_side.start()
    out[:, columns(col)] = pieces[col]
    out_y.wait_recv()
    other = pieces.at[across]
    out_corner = remote(other, other, send_out.at[2], recv_out.at[2], (row, partner))
    out_corner.start()
    out[:, columns(across)] = pieces[across]
    out_side.wait_recv()
    out[:, columns(partner)] = pieces[partner]
    for k in order:
        to_side[k].wait_send()
        to_own[k].wait_send()
        to_y[k].wait_send()
        if k:
            to_ep[k].wait_send()
    out_corner.wait_recv()
    out[:, columns(corner)] = pieces[corner]
    out_y.wait_send()
    out_side.wait_send()
    out_corner.wait_send()


def combine(part, weights):
    count, capacity, width = part.shape
    rows = weights.shape[0]
    quarter = width // 4
    chunk = pltpu.VMEM((count, capacity, quarter), jnp.bfloat16)
    return pl.pallas_call(
        lambda *refs: combine_kernel(count, *refs),
        out_shape=jax.ShapeDtypeStruct((rows, width), jnp.bfloat16),
        in_specs=[pl.BlockSpec(memory_space=pltpu.VMEM)] * 2,
        out_specs=pl.BlockSpec(memory_space=pltpu.VMEM),
        scratch_shapes=[chunk] * 6
        + [
            pltpu.VMEM((4, rows, quarter), jnp.bfloat16),
            pltpu.SemaphoreType.DMA((4, count)),
            pltpu.SemaphoreType.DMA((4, count)),
            pltpu.SemaphoreType.DMA((3,)),
            pltpu.SemaphoreType.DMA((3,)),
        ],
        compiler_params=pltpu.CompilerParams(
            collective_id=1, has_side_effects=True, vmem_limit_bytes=VMEM_LIMIT
        ),
        cost_estimate=pl.CostEstimate(flops=10**9, bytes_accessed=2**21, transcendentals=0),
        name="combine",
    )(part, weights)


def expert_half_kernels(
    second_batch, expert_gain, expert_choice, route_scores, expert_gate, expert_up, expert_down,
    mixer_in, mixer_out,
):
    row_count, model_width = second_batch.shape
    experts = lax.axis_size("ep")
    capacity = 4 * row_count // experts
    share = capacity // 4
    normed = rms_scale(second_batch, expert_gain)
    names = jnp.arange(experts, dtype=jnp.int32)
    is_first = expert_choice[:, 0:1] == names[None, :]
    is_second = expert_choice[:, 1:2] == names[None, :]
    named = is_first | is_second
    rows = jnp.arange(row_count, dtype=jnp.int32)
    before = (rows[None, :] < rows[:, None]).astype(jnp.bfloat16)
    rank = jnp.dot(
        before, named.astype(jnp.bfloat16), preferred_element_type=jnp.float32
    ).astype(jnp.int32)
    rank = jnp.where(named, rank, -1)
    places = lax.axis_index("tp") * share + jnp.arange(share, dtype=jnp.int32)
    pick = (rank.T[:, None, :] == places[None, :, None]).astype(jnp.bfloat16)
    portion = (
        jnp.dot(
            pick.reshape(experts * share, row_count), normed, preferred_element_type=jnp.float32
        )
        .astype(jnp.bfloat16)
        .reshape(experts, share, model_width)
    )
    arrived, full_in, full_out = dispatch(portion, mixer_in, mixer_out)
    incoming = arrived.reshape(experts * capacity, model_width)
    gate_part = jnp.dot(incoming, expert_gate[0], preferred_element_type=jnp.float32)
    up_part = jnp.dot(incoming, expert_up[0], preferred_element_type=jnp.float32)
    hidden = (jax.nn.silu(gate_part) * up_part).astype(jnp.bfloat16)
    part = jnp.dot(hidden, expert_down[0], preferred_element_type=jnp.float32).astype(
        jnp.bfloat16
    )
    weight_first = jax.nn.sigmoid(route_scores[:, 0] - route_scores[:, 1])[:, None]
    weight = jnp.where(is_first, weight_first, 1.0 - weight_first)
    slot = jnp.arange(capacity, dtype=jnp.int32)
    table = jnp.where(rank[:, :, None] == slot[None, None, :], weight[:, :, None], 0.0)
    blended = combine(
        part.reshape(experts, capacity, model_width),
        table.reshape(row_count, experts * capacity),
    )
    return blended, full_in, full_out


def per_device(
    first_batch,
    mixer_gain,
    mixer_in,
    group_maps,
    pool_scale,
    mixer_out,
    second_batch,
    expert_gain,
    expert_choice,
    route_scores,
    expert_gate,
    expert_up,
    expert_down,
):
    routed = (
        second_batch, expert_gain, expert_choice, route_scores, expert_gate, expert_up, expert_down
    )
    if lax.axis_size("tp") == 4 and lax.axis_size("ep") <= 8:
        experts_second, full_in, full_out = expert_half_kernels(*routed, mixer_in, mixer_out)
    else:
        experts_second = expert_half(*routed)
        full_in = lax.all_gather(mixer_in, "tp", axis=1, tiled=True)
        full_out = lax.all_gather(mixer_out, "tp", axis=0, tiled=True)
    mixed_first = mixer_half(
        first_batch, mixer_gain, full_in, group_maps, pool_scale, full_out
    )
    return (mixed_first, experts_second)


def solution(mesh):
    placed = (
        P(("ep", "tp"), None),
        P(),
        P(None, "tp"),
        P(),
        P(),
        P("tp", None),
        P("ep", None),
        P(),
        P("ep", None),
        P("ep", None),
        P("ep", None, "tp"),
        P("ep", None, "tp"),
        P("ep", "tp", None),
    )
    return jax.shard_map(
        per_device,
        mesh=mesh,
        in_specs=placed,
        out_specs=(P(("ep", "tp"), None), P("ep", None)),
        check_vma=False,
    )
```
